32 devices in a mesh: ep: 8 (over z, core), tp: 4 (over y, x).
Axes of the slice: x: 2, y: 2, z: 4, core: 2. Of those that a mesh axis runs over, the one named last changes fastest.
Arguments:
- query_rows: bfloat16 [4096, 2048], P('ep', 'tp'), may hold values from -6 to 6
- key_rows: bfloat16 [4096, 2048], P('ep', 'tp'), may hold values from -6 to 6
- value_rows: bfloat16 [4096, 4096], P('ep', 'tp'), may hold values from -6 to 6
- in_gate: float32 [16, 4096], P('tp', 'ep'), may hold values from -120 to 120
- forget_gate: float32 [16, 4096], P('tp', 'ep'), may hold values from -2 to 20
- out_gate: bfloat16 [4096, 4096], P('ep', 'tp'), may hold values from -6 to 6
- head_gain: float32 [4096], P('tp'), may hold values from 0.1 to 1.9
- mix_weight: bfloat16 [4096, 4096], P(None, 'tp'), may hold values from -0.09375 to 0.09375
- expert_input: bfloat16 [2048, 4096], P('ep', 'tp'), may hold values from -30 to 30
- routes: int32 [2048, 2], P('ep'), may hold values from 0 to 7, all different within a row; in each aligned block of 256 rows (0 to 255, 256 to 511, ...) at most 128 rows name the same one
- route_weight: float32 [2048, 2], P('ep'), may hold values from 0.25 to 1.25
- gate_weight: bfloat16 [8, 1024, 4096], P('ep', 'tp'), may hold values from -0.09375 to 0.09375
- up_weight: bfloat16 [8, 1024, 4096], P('ep', 'tp'), may hold values from -0.09375 to 0.09375
- down_weight: bfloat16 [8, 1024, 4096], P('ep', None, 'tp'), may hold values from -0.1875 to 0.1875
Outputs:
- mixer_out: bfloat16 [4096, 4096], P('ep', 'tp')
- expert_out: bfloat16 [2048, 4096], P('ep', 'tp')
The draws below stay inside these ranges and needn't reach their ends.
Inputs may be any that keep to these rules, and one draw needn't show every extreme that they name: `routes`: each row names 2 different experts. In the rows of one device no expert is named by more than 128 rows, and in the rows of some device an expert is named by exactly 128 rows.
All inputs are finite; a program needn't handle non-finite values.
Results may differ from the reference program's by a relative error of at most 0.0057.
Values may be sent and summed in bfloat16 or wider, within the bound.
No kernel may reach another device: no remote copies, remote signals or barrier semaphores. Data moves between devices by JAX's collectives and lax.ppermute only.
A program may use at most 128 MiB of HBM per device.

```python
import math
import jax
import jax.numpy as jnp
import numpy as np
from jax import lax

D = 4096
HEADS = 16
QK = 128
FF = 1024
TOP = 2
BLOCK = 64
ROWS_A = 512
ROWS_B = 256
TOKENS_A = 4096
TOKENS_B = 2048
EXPERTS = 8
CAP = 128
N_EP = 8


def draw_in_gate(key, part):
    base = jnp.clip(jax.random.normal(jax.random.fold_in(key, 11), (HEADS, TOKENS_A), jnp.float32), -4.0, 4.0)
    return base


def draw_forget_gate(key, part):
    slow_share = 0.5
    slow_heads = jax.random.bernoulli(jax.random.fold_in(key, 21), slow_share, (HEADS, 1))
    level = jnp.where(slow_heads, math.log(TOKENS_A) + 0.5, 3.5)
    span_total = TOKENS_A // ROWS_A
    drift = jax.random.uniform(jax.random.fold_in(key, 22), (HEADS, span_total), jnp.float32, -1.0, 1.0)
    noise = 0.7 * jnp.clip(jax.random.normal(jax.random.fold_in(key, 23), (HEADS, TOKENS_A), jnp.float32), -4.0, 4.0)
    return level + jnp.repeat(drift, ROWS_A, axis=1) + noise


def draw_expert_input(key, part):
    row_scale = jnp.exp(jax.random.uniform(jax.random.fold_in(key, 31), (TOKENS_B, 1), jnp.float32, -0.7, 0.7))
    base = jnp.clip(jax.random.normal(jax.random.fold_in(key, 34), (TOKENS_B, D), jnp.float32), -4.0, 4.0)
    return (base * row_scale).astype(jnp.bfloat16)


def steps_of(rng, extent, split, low, high):
    loudness, own = 1.0, jax.random.fold_in(rng, 6)
    for axis_at, shards_of in split:
        steps = jnp.exp(jax.random.uniform(jax.random.fold_in(own, axis_at), (shards_of,), jnp.float32, low / len(split), high / len(split)))
        loudness = loudness * jnp.repeat(steps, extent[axis_at] // shards_of).reshape([-1 if axis == axis_at else 1 for axis in range(len(extent))])
    return loudness


def deal_out(key, own, number, rows, count, top, bound, slope):
    order = jax.random.permutation(key, count)
    packed, usual = load_shares(count, rows * top, bound, slope, True), load_shares(count, rows * top, bound, slope, False)
    places = jnp.arange(count)

    def named(tallies, offset_by):
        used = int((tallies > 0).sum())
        fixed = max(1, used // 4)
        shifted = fixed + (places - fixed + offset_by * (used - fixed)) % max(1, count - fixed)
        return jnp.zeros((count,), jnp.int32).at[order[jnp.where(places < fixed, places, shifted)]].set(jnp.asarray(tallies, jnp.int32))

    tallies = jnp.where(number % 4 == 0, named(packed, number // 4), named(usual, number - number // 4 - 1))
    mixed = jax.random.permutation(jax.random.fold_in(own, 3), count)
    donor, taker = mixed[0:count // 2 * 2:2], mixed[1:count // 2 * 2:2]
    room = jnp.minimum(tallies[donor] - 1, bound - tallies[taker]) // 2
    room = jnp.where((donor == order[0]) | (taker == order[0]) | (tallies[taker] == 0), 0, jnp.maximum(room, 0))
    shifted = jax.random.randint(jax.random.fold_in(own, 4), (count // 2,), 0, 1 << 20) % (room + 1)
    tallies = tallies.at[donor].add(-shifted).at[taker].add(shifted)
    labels = jnp.searchsorted(jnp.cumsum(tallies), jnp.arange(rows * top), side="right").astype(jnp.int32)
    listing = labels.reshape(top, rows).T
    listing = listing[jax.random.permutation(jax.random.fold_in(own, 1), rows)]
    offset_by = jax.random.randint(jax.random.fold_in(own, 2), (rows, 1), 0, top)
    return jnp.take_along_axis(listing, (jnp.arange(top)[None, :] + offset_by) % top, axis=1)


def load_shares(amount, total, bound, lean, full):
    weights = [(1 << 20) // math.isqrt(grade ** lean) + 1 for grade in range(1, amount + 1)]
    largest = bound if full else min(bound, max(-(-total // amount), total * weights[0] // sum(weights)))
    least = 1 if total - largest >= amount - 1 else 0
    given, rest = [largest] + [least] * (amount - 1), total - largest - least * (amount - 1)
    while rest > 0:
        free = [i for i in range(1, amount) if given[i] < largest] or [i for i in range(1, amount) if given[i] < bound]
        mass, remaining = sum([weights[i] for i in free]), rest
        for i in free:
            extra = min(bound - given[i], max(1, remaining * weights[i] // mass), rest)
            given[i] = given[i] + extra
            rest = rest - extra
    return np.array(given)


def centred(key, dims, scale, bound, cuts=(), kind=jnp.bfloat16):
    level = steps_of(key, dims, cuts, -0.22, 0.18) if cuts else 1.0
    entries = jax.random.normal(key, dims, jnp.float32) * scale * level
    return jnp.minimum(jnp.maximum(entries, -bound), bound).astype(kind)


def setup_inputs(seed: int = 0) -> dict:
    key_of = jax.random.split(jax.random.key(seed), 15)
    query_rows = centred(key_of[0], (TOKENS_A, HEADS * QK), 1.0, 6.0, ((0, 8), (1, 4)))
    key_rows = centred(key_of[1], (TOKENS_A, HEADS * QK), 1.0, 6.0, ((0, 8), (1, 4)))
    value_rows = centred(key_of[2], (TOKENS_A, D), 1.0, 6.0, ((0, 8), (1, 4)))
    in_gate = draw_in_gate(jax.random.fold_in(key_of[14], 71), 0)
    forget_gate = draw_forget_gate(jax.random.fold_in(key_of[14], 71), 0)
    out_gate = centred(key_of[5], (TOKENS_A, D), 1.0, 6.0, ((0, 8), (1, 4)))
    head_gain = jnp.clip(1.0 + 0.18 * jax.random.normal(key_of[6], (D,), jnp.float32), 0.1, 1.9)
    mix_weight = centred(key_of[7], (D, D), D ** -0.5, 0.09375, ((1, 4),))
    expert_input = draw_expert_input(jax.random.fold_in(key_of[14], 71), 0)
    routes_keys = jax.random.split(jax.random.fold_in(key_of[9], 1), TOKENS_B // ROWS_B)
    routes_turns = jax.random.permutation(jax.random.fold_in(key_of[9], 3), TOKENS_B // ROWS_B)
    routes = jax.vmap(lambda own, number: deal_out(jax.random.fold_in(key_of[9], 2), own, number, ROWS_B, EXPERTS, TOP, CAP, 1))(routes_keys, routes_turns).reshape((TOKENS_B, TOP))
    route_weight = jnp.clip(0.25 + 1.0 * jax.random.uniform(key_of[10], (TOKENS_B, TOP), jnp.float32) ** steps_of(key_of[10], (TOKENS_B, TOP), ((0, 8),), -0.2, 0.2), 0.25, 1.25)
    gate_weight = centred(key_of[11], (EXPERTS, FF, D), D ** -0.5, 0.09375, ((0, 8), (1, 4)))
    up_weight = centred(key_of[12], (EXPERTS, FF, D), D ** -0.5, 0.09375, ((0, 8), (1, 4)))
    down_weight = centred(key_of[13], (EXPERTS, FF, D), FF ** -0.5, 0.1875, ((0, 8), (2, 4)))
    return dict(query_rows=query_rows, key_rows=key_rows, value_rows=value_rows, in_gate=in_gate, forget_gate=forget_gate, out_gate=out_gate, head_gain=head_gain, mix_weight=mix_weight, expert_input=expert_input, routes=routes, route_weight=route_weight, gate_weight=gate_weight, up_weight=up_weight, down_weight=down_weight)


EPSILON = 1e-06
LOG_FLOOR = -1e+30
HIGHEST_PRECISION = lax.Precision.HIGHEST

def combine(first_part, second_part):
    decay_first, max_first, memory_first, normal_first = first_part
    decay_second, max_second, memory_second, normal_second = second_part
    running_max = jnp.maximum(decay_second + max_first, max_second)
    keep_first = jnp.exp(decay_second + max_first - running_max)
    keep_second = jnp.exp(max_second - running_max)
    memory = keep_first[..., None, None] * memory_first + keep_second[..., None, None] * memory_second
    normalizer = keep_first[..., None] * normal_first + keep_second[..., None] * normal_second
    return (decay_first + decay_second, running_max, memory, normalizer)

def identity_state(head_count, key_width, value_width):
    return (jnp.zeros((head_count,), jnp.float32), jnp.full((head_count,), LOG_FLOOR, jnp.float32), jnp.zeros((head_count, key_width, value_width), jnp.float32), jnp.zeros((head_count, key_width), jnp.float32))

def halfprod(form, left, right):
    return jnp.einsum(form, left.astype(jnp.float32), right.astype(jnp.float32), precision=HIGHEST_PRECISION)

def prepare(query_heads, key_heads, value_heads, in_gate, forget_gate):
    head_count, length, key_width = query_heads.shape
    block_count = length // BLOCK
    query_blocks = query_heads.reshape(head_count, block_count, BLOCK, key_width)
    key_blocks = key_heads.reshape(head_count, block_count, BLOCK, key_width)
    value_blocks = value_heads.reshape(head_count, block_count, BLOCK, value_heads.shape[-1])
    log_input = in_gate.reshape(head_count, block_count, BLOCK)
    cumulative = jnp.cumsum(jax.nn.log_sigmoid(forget_gate).reshape(head_count, block_count, BLOCK), axis=-1)
    block_decay = cumulative[..., -1]
    weight_log = block_decay[..., None] - cumulative + log_input
    block_max = lax.optimization_barrier(jnp.max(weight_log, axis=-1))
    weighted = key_blocks.astype(jnp.float32) * jnp.exp(weight_log - block_max[..., None])[..., None]
    normalizer = lax.optimization_barrier(jnp.sum(weighted, axis=2))
    memory = halfprod('hcsk,hcsv->hckv', weighted.astype(jnp.bfloat16), value_blocks)
    return ((query_blocks, key_blocks, value_blocks, log_input, cumulative), (block_decay, block_max, memory, normalizer))

def prefix(summary, initial):
    leading = jax.tree.map(lambda tensor: jnp.moveaxis(tensor, 1, 0), summary)

    def advance(running, current):
        return (combine(running, current), running)
    final_state, before = lax.scan(advance, initial, leading)
    return (final_state, jax.tree.map(lambda tensor: jnp.moveaxis(tensor, 0, 1), before))

def block_outputs(blocked, before):
    query_blocks, key_blocks, value_blocks, log_input, cumulative = blocked
    prior_max, prior_memory, prior_normal = (before[1], before[2], before[3])
    block_len = cumulative.shape[-1]
    scale = query_blocks.shape[-1] ** (-0.5)
    causal = jnp.tril(jnp.ones((block_len, block_len), dtype=bool))
    log_decay = jnp.where(causal, cumulative[..., :, None] - cumulative[..., None, :] + log_input[..., None, :], -jnp.inf)
    log_inter = cumulative + prior_max[..., None]
    top_value = jnp.maximum(log_inter, lax.optimization_barrier(jnp.max(log_decay, axis=-1)))
    scores = halfprod('hctk,hcsk->hcts', query_blocks, key_blocks) * scale * jnp.exp(log_decay - top_value[..., None])
    carried = jnp.exp(log_inter - top_value) * scale
    query_wide = query_blocks.astype(jnp.float32)
    numerator = carried[..., None] * jnp.einsum('hctk,hckv->hctv', query_wide, prior_memory, precision=HIGHEST_PRECISION) + halfprod('hcts,hcsv->hctv', scores.astype(jnp.bfloat16), value_blocks)
    denominator = carried * jnp.einsum('hctk,hck->hct', query_wide, prior_normal, precision=HIGHEST_PRECISION) + lax.optimization_barrier(jnp.sum(scores, axis=-1))
    return numerator / jnp.maximum(jnp.abs(denominator), jnp.exp(-top_value))[..., None]

def finish(head_values, out_gate, head_gain):
    head_count, block_count, block_len, value_width = head_values.shape
    per_head = jnp.transpose(head_values, (1, 2, 0, 3)).reshape(block_count * block_len, head_count, value_width)
    per_head = per_head * lax.rsqrt(lax.optimization_barrier(jnp.mean(per_head * per_head, axis=-1, keepdims=True)) + EPSILON)
    per_head = per_head.reshape(block_count * block_len, head_count * value_width) * head_gain
    per_head = per_head * jax.nn.sigmoid(out_gate.astype(jnp.float32))
    return per_head.astype(jnp.bfloat16)

def reference(query_rows, key_rows, value_rows, in_gate, forget_gate, out_gate, head_gain, mix_weight, expert_input, routes, route_weight, gate_weight, up_weight, down_weight):
    length = query_rows.shape[0]
    head_count = in_gate.shape[0]
    key_width = query_rows.shape[1] // head_count
    value_width = value_rows.shape[1] // head_count
    query_heads = query_rows.reshape(length, head_count, key_width).transpose(1, 0, 2)
    key_heads = key_rows.reshape(length, head_count, key_width).transpose(1, 0, 2)
    value_heads = value_rows.reshape(length, head_count, value_width).transpose(1, 0, 2)

    def one_head(current):
        query_one, key_one, value_one, input_one, forget_one = current
        blocked, summary = prepare(query_one[None], key_one[None], value_one[None], input_one[None], forget_one[None])
        final_state, before = prefix(summary, identity_state(1, key_width, value_width))
        return block_outputs(blocked, before)[0]
    head_values = lax.map(one_head, (query_heads, key_heads, value_heads, in_gate, forget_gate))
    mixed_heads = finish(head_values, out_gate, head_gain)
    mixer_out = jnp.dot(mixed_heads, mix_weight, preferred_element_type=jnp.float32).astype(jnp.bfloat16)
    squares = lax.optimization_barrier(jnp.sum(jnp.square(expert_input.astype(jnp.float32)), axis=-1))
    inverse_rms = lax.rsqrt(squares / D + EPSILON)
    slot_total = N_EP * CAP

    def one_expert(running, expert):
        matched = routes == expert
        picked = jnp.any(matched, axis=1)
        row_index = jnp.nonzero(picked, size=slot_total, fill_value=0)[0].astype(jnp.int32)
        count = jnp.sum(picked.astype(jnp.int32))
        is_valid = (jnp.arange(slot_total, dtype=jnp.int32) < count).astype(jnp.float32)
        weight = lax.optimization_barrier(jnp.sum(jnp.where(matched, route_weight, 0.0), axis=1))
        chosen = expert_input[row_index]
        row_scale = inverse_rms[row_index][:, None]
        gate_value = jnp.dot(chosen, gate_weight[expert].T, preferred_element_type=jnp.float32) * row_scale
        up_value = jnp.dot(chosen, up_weight[expert].T, preferred_element_type=jnp.float32) * row_scale
        hidden = (jax.nn.silu(gate_value) * up_value).astype(jnp.bfloat16)
        expert_rows = jnp.dot(hidden, down_weight[expert], preferred_element_type=jnp.float32).astype(jnp.bfloat16)
        term = expert_rows.astype(jnp.float32) * (weight[row_index] * is_valid)[:, None]
        return (running.at[row_index].add(term), None)
    total, _ = lax.scan(one_expert, jnp.zeros((TOKENS_B, D), jnp.float32), jnp.arange(EXPERTS, dtype=jnp.int32))
    return (mixer_out, total.astype(jnp.bfloat16))
```

```python
import jax
import jax.numpy as jnp
from jax import lax
from jax.experimental import pallas as pl
from jax.experimental.pallas import tpu as pltpu
from jax.sharding import PartitionSpec as P

EPSILON = 1e-06
LOG_FLOOR = -1e30
BF16 = jnp.bfloat16
F32 = jnp.float32
PAD = 16


def whole(shape):
    return pl.BlockSpec(shape, lambda *_: (0,) * len(shape))


def params(megabytes=40):
    return pltpu.CompilerParams(vmem_limit_bytes=megabytes << 20)


def cost(flops, moved):
    return pl.CostEstimate(flops=int(flops), bytes_accessed=int(moved), transcendentals=0)


def dot(left, right, left_dim=1, right_dim=0):
    return lax.dot_general(
        left, right, (((left_dim,), (right_dim,)), ((), ())), preferred_element_type=F32
    )


def split_two(value):
    high = value.astype(BF16)
    return high, (value - high.astype(F32)).astype(BF16)


def swap(value, axis, bit):
    count = lax.axis_size(axis)
    return lax.ppermute(value, axis, [(at, at ^ bit) for at in range(count)])


def spread(value, axis, bits):
    pieces = {0: value}
    for bit in bits:
        for at in list(pieces):
            pieces[at ^ bit] = swap(pieces[at], axis, bit)
    return [pieces[at] for at in range(len(pieces))]


def scan_lanes(row, join, neutral):
    lanes = row.shape[1]
    at = lax.broadcasted_iota(jnp.int32, row.shape, 1)
    step = 1
    while step < lanes:
        row = join(row, jnp.where(at >= step, pltpu.roll(row, step, 1), neutral))
        step *= 2
    return row


def decay_rows(in_gate_ref, forget_gate_ref, head):
    forget = forget_gate_ref[pl.ds(head, 1), :]
    log_input = in_gate_ref[pl.ds(head, 1), :]
    log_forget = jnp.minimum(forget, 0.0) - jnp.log1p(jnp.exp(-jnp.abs(forget)))
    log_forget = jnp.broadcast_to(log_forget, (8, log_forget.shape[1]))
    cumulative = scan_lanes(log_forget, jnp.add, 0.0)
    return cumulative, jnp.broadcast_to(log_input, cumulative.shape)


def tall(row):
    return jnp.transpose(jnp.broadcast_to(row, (128, row.shape[1])))


def summary_kernel(key_ref, value_ref, in_gate_ref, forget_gate_ref, out_ref):
    head = pl.program_id(0)
    cumulative, log_input = decay_rows(in_gate_ref, forget_gate_ref, head)
    length = cumulative.shape[1]
    key_width = key_ref.shape[1]
    value_width = value_ref.shape[1]
    decay = cumulative[:, length - 1 : length]
    weight_log = decay - cumulative + log_input
    top = jnp.max(weight_log, axis=1, keepdims=True)
    weight = jnp.exp(weight_log - top)
    weight_tall = tall(weight[0:1])[:, 0:1]
    weighted = key_ref[...].astype(F32) * weight_tall
    normal = jnp.sum(weighted, axis=0, keepdims=True)
    memory = dot(weighted.astype(BF16), value_ref[...], 0, 0)
    out_ref[0, 0:key_width, :] = memory.astype(BF16)
    normal_high, normal_low = split_two(normal)
    lane = lax.broadcasted_iota(jnp.int32, (1, value_width), 1)

    def limbs(number, base):
        row = jnp.zeros((1, value_width), F32)
        for at in range(3):
            part = number.astype(BF16).astype(F32)
            number = number - part
            row = row + jnp.where(lane == base + at, part, 0.0)
        return row

    scalars = limbs(decay[0:1], 0) + limbs(top[0:1], 3)
    sub = lax.broadcasted_iota(jnp.int32, (PAD, value_width), 0)
    both = jnp.concatenate([normal_high.astype(F32), normal_low.astype(F32)], axis=1)
    if 2 * key_width < value_width:
        both = jnp.pad(both, ((0, 0), (0, value_width - 2 * key_width)))
    tail = jnp.where(sub == 0, both, jnp.where(sub == 1, scalars, 0.0))
    out_ref[0, key_width : key_width + PAD, :] = tail.astype(BF16)


def summarise(key_rows, value_rows, in_gate, forget_gate):
    heads, length = in_gate.shape
    key_width = key_rows.shape[1] // heads
    value_width = value_rows.shape[1] // heads
    return pl.pallas_call(
        summary_kernel,
        grid=(heads,),
        in_specs=[
            pl.BlockSpec((length, key_width), lambda h: (0, h)),
            pl.BlockSpec((length, value_width), lambda h: (0, h)),
            whole(in_gate.shape),
            whole(forget_gate.shape),
        ],
        out_specs=pl.BlockSpec((1, key_width + PAD, value_width), lambda h: (h, 0, 0)),
        out_shape=jax.ShapeDtypeStruct((heads, key_width + PAD, value_width), BF16),
        compiler_params=params(),
        cost_estimate=cost(
            2 * length * key_width * value_width * heads, 2 * key_rows.size + 2 * value_rows.size
        ),
        name="summary",
    )(key_rows, value_rows, in_gate, forget_gate)


def heads_kernel(
    place_ref,
    states_ref,
    query_ref,
    key_ref,
    value_ref,
    in_gate_ref,
    forget_gate_ref,
    out_gate_ref,
    gain_ref,
    *rest,
):
    out_refs, memory_ref = rest[:-1], rest[-1]
    head = pl.program_id(0)
    mine = place_ref[0]
    length, key_width = query_ref.shape
    value_width = value_ref.shape[1]
    memory_ref[...] = jnp.zeros(memory_ref.shape, F32)

    def turn(position, carry):
        running_max, normal = carry
        state = states_ref.at[position ^ mine, 0]
        tail = state[key_width : key_width + PAD, :].astype(F32)
        added = tail[0:1, 0:key_width] + tail[0:1, key_width : 2 * key_width]
        decay = (tail[1:2, 0:1] + tail[1:2, 1:2]) + tail[1:2, 2:3]
        top = (tail[1:2, 3:4] + tail[1:2, 4:5]) + tail[1:2, 5:6]
        new_max = jnp.maximum(decay + running_max, top)
        keep = jnp.exp(decay + running_max - new_max)
        gain = jnp.exp(top - new_max)
        memory_ref[...] = keep * memory_ref[...] + gain * state[0:key_width, :].astype(F32)
        return new_max, keep * normal + gain * added

    prior_max, prior_normal = lax.fori_loop(
        0, mine, turn, (jnp.full((1, 1), LOG_FLOOR, F32), jnp.zeros((1, key_width), F32))
    )
    memory_high, memory_low = split_two(memory_ref[...])

    cumulative, log_input = decay_rows(in_gate_ref, forget_gate_ref, head)
    source = log_input - cumulative
    bound = jnp.maximum(scan_lanes(source, jnp.maximum, LOG_FLOOR), prior_max)
    sub = lax.broadcasted_iota(jnp.int32, (128, length), 0)
    columns = jnp.transpose(jnp.where(sub < 64, bound[0:1], cumulative[0:1]))
    scale = key_width ** (-0.5)
    parts = len(out_refs)
    rows = length // parts
    for part, out_ref in enumerate(out_refs):
        low, high = part * rows, (part + 1) * rows
        bound_tall = columns[low:high, 0:1]
        cumulative_tall = columns[low:high, 64:65]
        query = query_ref[low:high, :]
        keys = key_ref[0:high, :]
        gap = source[0:1, 0:high] - bound_tall
        at_row = lax.broadcasted_iota(jnp.int32, (rows, high), 0) + low
        at_lane = lax.broadcasted_iota(jnp.int32, (rows, high), 1)
        gap = jnp.where(at_lane <= at_row, gap, LOG_FLOOR)
        scores = dot(query, keys, 1, 1) * scale * jnp.exp(gap)
        carried = jnp.exp(prior_max - bound_tall) * scale
        inter = dot(query, memory_high) + dot(query, memory_low)
        numerator = carried * inter + dot(scores.astype(BF16), value_ref[0:high, :])
        reach = jnp.sum(query.astype(F32) * prior_normal, axis=1, keepdims=True)
        denominator = carried * reach + jnp.sum(scores, axis=1, keepdims=True)
        floor = jnp.exp(-(cumulative_tall + bound_tall))
        values = numerator / jnp.maximum(jnp.abs(denominator), floor)
        mean = jnp.mean(values * values, axis=1, keepdims=True)
        values = values * lax.rsqrt(mean + EPSILON) * gain_ref[...]
        gate = out_gate_ref[low:high, :].astype(F32)
        out_ref[...] = (values * jax.nn.sigmoid(gate)).astype(BF16)


def head_outputs(
    place, states, query_rows, key_rows, value_rows, in_gate, forget_gate, out_gate, gain, parts
):
    heads, length = in_gate.shape
    key_width = key_rows.shape[1] // heads
    value_width = value_rows.shape[1] // heads
    rows = length // parts

    def column(width):
        return pl.BlockSpec((length, width), lambda h, _: (0, h))

    return pl.pallas_call(
        heads_kernel,
        grid_spec=pltpu.PrefetchScalarGridSpec(
            num_scalar_prefetch=1,
            grid=(heads,),
            in_specs=[
                pl.BlockSpec(
                    (states.shape[0], 1) + states.shape[2:], lambda h, _: (0, h, 0, 0)
                ),
                column(key_width),
                column(key_width),
                column(value_width),
                whole(in_gate.shape),
                whole(forget_gate.shape),
                column(value_width),
                pl.BlockSpec((1, value_width), lambda h, _: (0, h)),
            ],
            out_specs=[pl.BlockSpec((rows, value_width), lambda h, _: (0, h))] * parts,
            scratch_shapes=[pltpu.VMEM((key_width, value_width), F32)],
        ),
        out_shape=[jax.ShapeDtypeStruct((rows, value_rows.shape[1]), BF16)] * parts,
        compiler_params=params(),
        cost_estimate=cost(
            heads * length * length * (key_width + value_width) * 4,
            2 * (query_rows.size + key_rows.size + 3 * value_rows.size + states.size),
        ),
        name="heads",
    )(place, states, query_rows, key_rows, value_rows, in_gate, forget_gate, out_gate, gain)


def mix_kernel(place_ref, *refs):
    weight_ref, out_ref = refs[-2], refs[-1]
    count = weight_ref.shape[0] // refs[0].shape[1]
    width = refs[0].shape[1]
    rows = refs[0].shape[0]
    for part in range((len(refs) - 2) // count):
        total = None
        for at in range(count):
            start = pl.multiple_of((place_ref[1] ^ at) * width, width)
            term = dot(refs[part * count + at][...], weight_ref[pl.ds(start, width), :])
            total = term if total is None else total + term
        out_ref[part * rows : (part + 1) * rows, :] = total.astype(BF16)


def mix(place, halves, weight):
    flat = [piece for pieces in halves for piece in pieces]
    rows = sum(pieces[0].shape[0] for pieces in halves)
    depth, width = weight.shape
    block = min(width, 256)
    return pl.pallas_call(
        mix_kernel,
        grid_spec=pltpu.PrefetchScalarGridSpec(
            num_scalar_prefetch=1,
            grid=(width // block,),
            in_specs=[whole(piece.shape) for piece in flat]
            + [pl.BlockSpec((depth, block), lambda n, _: (0, n))],
            out_specs=pl.BlockSpec((rows, block), lambda n, _: (0, n)),
        ),
        out_shape=jax.ShapeDtypeStruct((rows, width), BF16),
        compiler_params=params(),
        cost_estimate=cost(2 * rows * depth * width, 2 * weight.size),
        name="mix",
    )(place, *flat, weight)


def pick_kernel(place_ref, *refs):
    out_ref = refs[-1]
    sources = refs[:-1]
    expert = place_ref[0].astype(F32)
    tokens = sources[0].shape[0] - PAD
    slots = out_ref.shape[0] // len(sources)
    before = lax.broadcasted_iota(jnp.int32, (tokens, tokens), 0)
    after = lax.broadcasted_iota(jnp.int32, (tokens, tokens), 1)
    earlier = jnp.where(before < after, 1.0, 0.0).astype(BF16)
    slot = lax.broadcasted_iota(jnp.int32, (slots, tokens), 0).astype(F32)
    for at, source in enumerate(sources):
        tail = source[tokens : tokens + PAD, 0:tokens].astype(F32)
        sub = lax.broadcasted_iota(jnp.int32, tail.shape, 0)
        named = jnp.where((sub < 2) & (tail == expert), 1.0, 0.0)
        match = jnp.sum(named, axis=0, keepdims=True)
        wide = jnp.broadcast_to(match, (16, tokens)).astype(BF16)
        position = dot(wide, earlier)[0:1]
        chosen = jnp.where((slot == position) & (match > 0.5), 1.0, 0.0).astype(BF16)
        picked = dot(chosen, source[0:tokens, :])
        out_ref[at * slots : (at + 1) * slots, :] = picked.astype(BF16)


def pick(place, sources, slots):
    width = sources[0].shape[1]
    return pl.pallas_call(
        pick_kernel,
        grid_spec=pltpu.PrefetchScalarGridSpec(
            num_scalar_prefetch=1,
            grid=(1,),
            in_specs=[whole(source.shape) for source in sources],
            out_specs=whole((len(sources) * slots, width)),
        ),
        out_shape=jax.ShapeDtypeStruct((len(sources) * slots, width), BF16),
        compiler_params=params(),
        cost_estimate=cost(4 * len(sources) * slots * sources[0].size, 4 * sources[0].size),
        name="pick",
    )(place, *sources)


def gate_kernel(place_ref, *refs):
    pieces = refs[:-4]
    gate_ref, up_ref, out_ref, scale_ref = refs[-4:]
    width = pieces[0].shape[1]
    depth = width * len(pieces)

    @pl.when(pl.program_id(0) == 0)
    def _():
        squares = None
        for piece in pieces:
            value = piece[...].astype(F32)
            term = jnp.sum(value * value, axis=1, keepdims=True)
            squares = term if squares is None else squares + term
        scale_ref[...] = jnp.broadcast_to(lax.rsqrt(squares / depth + EPSILON), scale_ref.shape)

    gate, up = None, None
    for at, piece in enumerate(pieces):
        start = pl.multiple_of((place_ref[1] ^ at) * width, width)
        value = piece[...]
        gate_term = dot(value, gate_ref[:, pl.ds(start, width)], 1, 1)
        up_term = dot(value, up_ref[:, pl.ds(start, width)], 1, 1)
        gate = gate_term if gate is None else gate + gate_term
        up = up_term if up is None else up + up_term
    scale = scale_ref[:, 0:1]
    gate = gate * scale
    out_ref[...] = (gate * jax.nn.sigmoid(gate) * (up * scale)).astype(BF16)


def gate_up(place, pieces, gate_weight, up_weight):
    rows = pieces[0].shape[0]
    hidden, depth = gate_weight.shape
    block = min(hidden, 128)
    return pl.pallas_call(
        gate_kernel,
        grid_spec=pltpu.PrefetchScalarGridSpec(
            num_scalar_prefetch=1,
            grid=(hidden // block,),
            in_specs=[whole(piece.shape) for piece in pieces]
            + [pl.BlockSpec((block, depth), lambda n, _: (n, 0))] * 2,
            out_specs=pl.BlockSpec((rows, block), lambda n, _: (0, n)),
            scratch_shapes=[pltpu.VMEM((rows, 128), F32)],
        ),
        out_shape=jax.ShapeDtypeStruct((rows, hidden), BF16),
        compiler_params=params(),
        cost_estimate=cost(4 * rows * hidden * depth, 4 * hidden * depth),
        name="gate_up",
    )(place, *pieces, gate_weight, up_weight)


def down_kernel(place_ref, *refs):
    pieces = refs[:-3]
    down_ref, first_ref, second_ref = refs[-3:]
    width = pieces[0].shape[1]
    rows = first_ref.shape[0]
    total = None
    for at, piece in enumerate(pieces):
        start = pl.multiple_of((place_ref[1] ^ at) * width, width)
        term = dot(piece[...], down_ref[pl.ds(start, width), :])
        total = term if total is None else total + term
    first_ref[...] = total[0:rows].astype(BF16)
    second_ref[...] = total[rows : 2 * rows].astype(BF16)


def down(place, pieces, weight):
    rows = pieces[0].shape[0]
    depth, width = weight.shape
    block = min(width, 512)
    half = pl.BlockSpec((rows // 2, block), lambda n, _: (0, n))
    return pl.pallas_call(
        down_kernel,
        grid_spec=pltpu.PrefetchScalarGridSpec(
            num_scalar_prefetch=1,
            grid=(width // block,),
            in_specs=[whole(piece.shape) for piece in pieces]
            + [pl.BlockSpec((depth, block), lambda n, _: (0, n))],
            out_specs=[half, half],
        ),
        out_shape=[jax.ShapeDtypeStruct((rows // 2, width), BF16)] * 2,
        compiler_params=params(),
        cost_estimate=cost(2 * rows * depth * width, 2 * depth * width),
        name="down",
    )(place, *pieces, weight)


def gather_kernel(place_ref, routes_ref, weight_ref, *refs):
    out_ref = refs[-1]
    returned = refs[:-1]
    tokens, fanout = routes_ref.shape
    slots = returned[0].shape[0]
    mine = place_ref[0]
    lane = lax.broadcasted_iota(jnp.int32, (tokens, 128), 1)
    routes = [routes_ref[:, at : at + 1] for at in range(fanout)]
    match = jnp.zeros((tokens, 128), F32)
    for route in routes:
        match = match + jnp.where(lane == route, 1.0, 0.0)
    before = lax.broadcasted_iota(jnp.int32, (tokens, tokens), 1)
    after = lax.broadcasted_iota(jnp.int32, (tokens, tokens), 0)
    earlier = jnp.where(before < after, 1.0, 0.0).astype(BF16)
    position = dot(earlier, match.astype(BF16))
    spots = [
        jnp.sum(jnp.where(lane == route, position, 0.0), axis=1, keepdims=True)
        for route in routes
    ]
    slot = lax.broadcasted_iota(jnp.int32, (tokens, slots), 1).astype(F32)
    total = jnp.zeros(out_ref.shape, F32)
    for at, piece in enumerate(returned):
        table = jnp.zeros((tokens, slots), F32)
        for number, (route, spot) in enumerate(zip(routes, spots)):
            hit = (slot == spot) & (route == (mine ^ at))
            table = table + jnp.where(hit, weight_ref[:, number : number + 1], 0.0)
        high, low = split_two(table)
        rows = piece[...]
        total = total + dot(high, rows) + dot(low, rows)
    out_ref[...] = total.astype(BF16)


def gather_back(place, routes, route_weight, returned):
    tokens = routes.shape[0]
    slots, width = returned[0].shape
    return pl.pallas_call(
        gather_kernel,
        grid_spec=pltpu.PrefetchScalarGridSpec(
            num_scalar_prefetch=1,
            grid=(1,),
            in_specs=[whole(routes.shape), whole(route_weight.shape)]
            + [whole(piece.shape) for piece in returned],
            out_specs=whole((tokens, width)),
        ),
        out_shape=jax.ShapeDtypeStruct((tokens, width), BF16),
        compiler_params=params(),
        cost_estimate=cost(
            4 * tokens * slots * width * len(returned), 2 * len(returned) * slots * width
        ),
        name="gather_back",
    )(place, routes, route_weight, *returned)


def body(
    query_rows,
    key_rows,
    value_rows,
    in_gate,
    forget_gate,
    out_gate,
    head_gain,
    mix_weight,
    expert_input,
    routes,
    route_weight,
    gate_weight,
    up_weight,
    down_weight,
):
    group = lax.axis_size("ep")
    lanes = lax.axis_size("tp")
    place = jnp.stack([lax.axis_index("ep"), lax.axis_index("tp")]).astype(jnp.int32)
    tokens, fanout = routes.shape
    slots = 2 * tokens * fanout // group
    chips = group // 2
    bits = [1 << at for at in range(lanes.bit_length() - 1)]
    orders = [bits, bits[::-1]]

    named = routes.T.astype(BF16)
    named = jnp.pad(named, ((0, PAD - fanout), (0, expert_input.shape[1] - tokens)))
    packed = jnp.concatenate([expert_input, named], axis=0)

    turns = [0] + [at for at in range(1, chips)]
    direct = [packed if at == 0 else swap(packed, "ep", 2 * at) for at in turns]
    sibling = [swap(piece, "ep", 1) for piece in direct]

    state = summarise(key_rows, value_rows, in_gate, forget_gate)
    states_direct = [state if at == 0 else swap(state, "ep", 2 * at) for at in range(chips)]

    returned = {}
    for number, at in enumerate(turns):
        chosen = pick(place, [direct[number], sibling[number]], slots)
        pieces = spread(chosen, "tp", orders[number % 2])
        hidden = gate_up(place, pieces, gate_weight[0], up_weight[0])
        hidden_pieces = spread(hidden, "tp", orders[(number + 1) % 2])
        first, second = down(place, hidden_pieces, down_weight[0])
        returned[2 * at] = first if at == 0 else swap(first, "ep", 2 * at)
        returned[2 * at + 1] = swap(second, "ep", 2 * at + 1)

    states = []
    for piece in states_direct:
        states += [piece, swap(piece, "ep", 1)]
    parts = 2
    halves = head_outputs(
        place,
        jnp.stack(states),
        query_rows,
        key_rows,
        value_rows,
        in_gate,
        forget_gate,
        out_gate,
        head_gain[None, :],
        parts,
    )
    spreads = [spread(half, "tp", orders[at % 2]) for at, half in enumerate(halves)]
    mixer_out = mix(place, spreads, mix_weight)
    expert_out = gather_back(
        place, routes, route_weight, [returned[at] for at in range(group)]
    )
    return (mixer_out, expert_out)


def solution(mesh):
    in_specs = (
        P("ep", "tp"),
        P("ep", "tp"),
        P("ep", "tp"),
        P("tp", "ep"),
        P("tp", "ep"),
        P("ep", "tp"),
        P("tp"),
        P(None, "tp"),
        P("ep", "tp"),
        P("ep", None),
        P("ep", None),
        P("ep", "tp", None),
        P("ep", "tp", None),
        P("ep", None, "tp"),
    )
    out_specs = (P("ep", "tp"), P("ep", "tp"))
    return jax.shard_map(body, mesh=mesh, in_specs=in_specs, out_specs=out_specs, check_vma=False)
```
